32 devices in a mesh: grp: 2 (over y), sp: 4 (over z), tp: 4 (over x, core).
Axes of the slice: x: 2, y: 2, z: 4, core: 2. Of those that a mesh axis runs over, the one named last changes fastest.
Arguments:
- query_nope: bfloat16 [2560, 1024], P(('grp', 'sp'), 'tp'), parts along dimension 0, may hold values from -12 to 12
- query_rope: bfloat16 [2560, 512], P(('grp', 'sp'), 'tp'), parts along dimension 0, may hold values from -48 to 48
- token_latent: bfloat16 [2560, 256], P(('grp', 'sp')), parts along dimension 0, may hold values from -6 to 6
- key_rope: bfloat16 [2560, 32], P(('grp', 'sp')), parts along dimension 0, may hold values from -48 to 48
- latent_norm_gain: float32 [256], replicated, may hold values from 0.1 to 1.9
- key_expand_weight: bfloat16 [256, 1024], replicated, may hold values from -0.375 to 0.375
- value_expand_weight: bfloat16 [256, 1024], replicated, may hold values from -0.375 to 0.375
- residual: bfloat16 [2560, 2048], P(('grp', 'sp')), parts along dimension 0, may hold values from -3 to 3
- out_weight: bfloat16 [1024, 2048], P('tp'), may hold values from -0.375 to 0.375
- ffn_gain: float32 [2048], replicated, may hold values from 0.1 to 1.9
- gate_weight: bfloat16 [2048, 5632], P('sp', 'tp'), may hold values from -0.125 to 0.125
- up_weight: bfloat16 [2048, 5632], P('sp', 'tp'), may hold values from -0.125 to 0.125
- down_weight: bfloat16 [5632, 2048], P('tp', 'sp'), may hold values from -0.078125 to 0.078125
Outputs:
- layer_output: bfloat16 [2560, 2048], P(('grp', 'sp', 'tp')), parts along dimension 0
The draws below stay inside these ranges and needn't reach their ends.
There are 2 independent parts, one for each index of `grp`. The reference program is written for one: setup_inputs(seed, part) draws one part's arguments, and reference() takes and returns one part's arrays. A program takes and returns all parts, laid end to end along the dimension named above; an argument that names none is the same for every part. Nothing has to cross between parts.
All inputs are finite; a program needn't handle non-finite values.
Results may differ from the reference program's by a relative error of at most 0.015.
Values may be sent and summed in bfloat16 or wider, within the bound.
A program may use at most 128 MiB of HBM per device.

```python
import math
import jax
import jax.numpy as jnp
from jax import lax

D = 2048
HEAD_COUNT = 16
UNROTATED_SIZE = 64
ROPE = 32
VALUE_SIZE = 64
LATENT_RANK = 256
FF = 5632
GRID_W = 64
TOKEN_COUNT = 1280
N_TP = 4


def rope_pair(key):
    base = jax.random.fold_in(key, 29)
    streams = jax.random.split(base, 2)
    key_rope = jax.random.normal(streams[0], (TOKEN_COUNT, ROPE), jnp.float32)
    query_rope = 2.5 * jax.random.normal(streams[1], (TOKEN_COUNT, HEAD_COUNT * ROPE), jnp.float32)
    return (jnp.clip(key_rope, -48.0, 48.0), jnp.clip(query_rope, -48.0, 48.0))


def draw_query_rope(key, part):
    return rope_pair(key)[1].astype(jnp.bfloat16)


def draw_key_rope(key, part):
    return rope_pair(key)[0].astype(jnp.bfloat16)


def level_of(stream_key, shape, shards, low, high):
    level, own = 1.0, jax.random.fold_in(stream_key, 6)
    for axis_at, shards_of in shards:
        heights = jnp.exp(jax.random.uniform(jax.random.fold_in(own, axis_at), (shards_of,), jnp.float32, low / len(shards), high / len(shards)))
        level = level * jnp.repeat(heights, shape[axis_at] // shards_of).reshape([-1 if axis == axis_at else 1 for axis in range(len(shape))])
    return level


def gaussian(key, extent, deviation, most, cuts=(), kind=jnp.bfloat16):
    loudness = level_of(key, extent, cuts, -0.22, 0.18) if cuts else 1.0
    result = jax.random.normal(key, extent, jnp.float32) * deviation * loudness
    return jnp.minimum(jnp.maximum(result, -most), most).astype(kind)


def setup_inputs(seed: int = 0, part: int = 0) -> dict:
    key_list = jax.random.split(jax.random.key(seed), 14)
    part_keys = jax.random.split(jax.random.fold_in(key_list[13], part), 14)
    return {
        "query_nope": gaussian(part_keys[0], (TOKEN_COUNT, HEAD_COUNT * UNROTATED_SIZE), 2.5, 12.0, ((0, 4), (1, 4))),
        "query_rope": draw_query_rope(jax.random.fold_in(jax.random.fold_in(key_list[13], part), 71), part),
        "token_latent": gaussian(part_keys[2], (TOKEN_COUNT, LATENT_RANK), 1.0, 6.0, ((0, 4),)),
        "key_rope": draw_key_rope(jax.random.fold_in(jax.random.fold_in(key_list[13], part), 71), part),
        "latent_norm_gain": jnp.clip(1.0 + 0.18 * jax.random.normal(key_list[4], (LATENT_RANK,), jnp.float32), 0.1, 1.9),
        "key_expand_weight": gaussian(key_list[5], (LATENT_RANK, HEAD_COUNT * UNROTATED_SIZE), LATENT_RANK ** -0.5, 0.375),
        "value_expand_weight": gaussian(key_list[6], (LATENT_RANK, HEAD_COUNT * VALUE_SIZE), LATENT_RANK ** -0.5, 0.375),
        "residual": gaussian(part_keys[7], (TOKEN_COUNT, D), 0.5, 3.0, ((0, 4),)),
        "out_weight": gaussian(key_list[8], (HEAD_COUNT * VALUE_SIZE, D), (HEAD_COUNT * VALUE_SIZE // 4) ** -0.5, 0.375, ((0, 4),)),
        "ffn_gain": jnp.clip(1.0 + 0.18 * jax.random.normal(key_list[9], (D,), jnp.float32), 0.1, 1.9),
        "gate_weight": gaussian(key_list[10], (D, FF), D ** -0.5, 0.125, ((0, 4), (1, 4))),
        "up_weight": gaussian(key_list[11], (D, FF), D ** -0.5, 0.125, ((0, 4), (1, 4))),
        "down_weight": gaussian(key_list[12], (FF, D), FF ** -0.5, 0.078125, ((0, 4), (1, 4))),
    }


def norm_rows(values, gain):
    wide = values.astype(jnp.float32)
    return wide * lax.rsqrt(lax.optimization_barrier(jnp.mean(wide * wide, axis=-1, keepdims=True)) + 1e-06) * gain.astype(jnp.float32)

def turn_heads(vectors, positions):
    tokens, heads, width = vectors.shape
    freqs = width // 4
    grid_pos = jnp.stack([positions // GRID_W, positions % GRID_W], axis=-1).astype(jnp.float32)
    inverse = jnp.power(10000.0, -jnp.arange(freqs, dtype=jnp.float32) / freqs)
    angles = grid_pos[:, :, None] * inverse
    cosine = jnp.cos(angles)[:, None]
    sine = jnp.sin(angles)[:, None]
    viewed = vectors.reshape(tokens, heads, 2, 2, freqs)
    first = viewed[..., 0, :]
    second = viewed[..., 1, :]
    turned = jnp.stack([first * cosine - second * sine, first * sine + second * cosine], axis=-2)
    return turned.reshape(tokens, heads, width)

def reference(query_nope, query_rope, token_latent, key_rope, latent_norm_gain, key_expand_weight, value_expand_weight, residual, out_weight, ffn_gain, gate_weight, up_weight, down_weight):
    tokens = query_nope.shape[0]
    positions = jnp.arange(tokens, dtype=jnp.int32)
    query_flat = query_nope.reshape(tokens, HEAD_COUNT, UNROTATED_SIZE)
    query_turned = turn_heads(query_rope.astype(jnp.float32).reshape(tokens, HEAD_COUNT, ROPE), positions).astype(jnp.bfloat16)
    latent_normed = norm_rows(token_latent, latent_norm_gain).astype(jnp.bfloat16)
    key_turned = turn_heads(key_rope.astype(jnp.float32)[:, None, :], positions)[:, 0].astype(jnp.bfloat16)
    key_nope = jnp.dot(latent_normed, key_expand_weight, preferred_element_type=jnp.float32).astype(jnp.bfloat16)
    key_nope = key_nope.reshape(tokens, HEAD_COUNT, UNROTATED_SIZE)
    head_values = jnp.dot(latent_normed, value_expand_weight, preferred_element_type=jnp.float32).astype(jnp.bfloat16)
    head_values = head_values.reshape(tokens, HEAD_COUNT, VALUE_SIZE)
    score_scale = (UNROTATED_SIZE + ROPE) ** (-0.5)
    block_rows = math.gcd(tokens, 512)
    keys_wide = key_nope.astype(jnp.float32)
    rope_wide = key_turned.astype(jnp.float32)
    values_wide = head_values.astype(jnp.float32)

    def one_block(blocks):
        query_block, turned_block = blocks
        scores = (jnp.einsum('qhd,khd->hqk', query_block.astype(jnp.float32), keys_wide) + jnp.einsum('qhd,kd->hqk', turned_block.astype(jnp.float32), rope_wide)) * score_scale
        highest = lax.optimization_barrier(jnp.max(scores, axis=-1, keepdims=True))
        raised = jnp.exp(scores - highest)
        totals = lax.optimization_barrier(jnp.sum(raised, axis=-1))
        rounded = lax.optimization_barrier(raised.astype(jnp.bfloat16)).astype(jnp.float32)
        summed = jnp.einsum('hqk,khd->qhd', rounded, values_wide)
        return (summed / totals.T[:, :, None]).astype(jnp.bfloat16)
    attended = lax.map(one_block, (query_flat.reshape(-1, block_rows, HEAD_COUNT, UNROTATED_SIZE), query_turned.reshape(-1, block_rows, HEAD_COUNT, ROPE)))
    attended = attended.reshape(tokens, HEAD_COUNT * VALUE_SIZE)
    head_cols = HEAD_COUNT // N_TP * VALUE_SIZE
    mixed = residual.astype(jnp.float32)
    for member in range(N_TP):
        partial_out = jnp.dot(attended[:, member * head_cols:(member + 1) * head_cols], out_weight[member * head_cols:(member + 1) * head_cols], preferred_element_type=jnp.float32).astype(jnp.bfloat16)
        mixed = mixed + partial_out.astype(jnp.float32)
    normed = norm_rows(mixed, ffn_gain).astype(jnp.bfloat16)
    gate = jnp.dot(normed, gate_weight, preferred_element_type=jnp.float32)
    up_part = jnp.dot(normed, up_weight, preferred_element_type=jnp.float32)
    hidden = (jax.nn.silu(gate) * up_part).astype(jnp.bfloat16)
    hidden_cols = FF // N_TP
    layer_output = mixed
    for member in range(N_TP):
        partial_out = jnp.dot(hidden[:, member * hidden_cols:(member + 1) * hidden_cols], down_weight[member * hidden_cols:(member + 1) * hidden_cols], preferred_element_type=jnp.float32).astype(jnp.bfloat16)
        layer_output = layer_output + partial_out.astype(jnp.float32)
    return layer_output.astype(jnp.bfloat16)
```

```python
import jax
import jax.numpy as jnp
from jax import lax
from jax.sharding import PartitionSpec as P

UNROTATED_SIZE = 64
ROPE = 32
VALUE_SIZE = 64
GRID_W = 64


def norm_rows(values, gain):
    wide = values.astype(jnp.float32)
    return wide * lax.rsqrt(jnp.mean(wide * wide, axis=-1, keepdims=True) + 1e-06) * gain


def turn_heads(vectors, positions):
    tokens, heads, width = vectors.shape
    freqs = width // 4
    grid_pos = jnp.stack([positions // GRID_W, positions % GRID_W], axis=-1).astype(jnp.float32)
    inverse = jnp.power(10000.0, -jnp.arange(freqs, dtype=jnp.float32) / freqs)
    angles = grid_pos[:, :, None] * inverse
    cosine = jnp.cos(angles)[:, None]
    sine = jnp.sin(angles)[:, None]
    viewed = vectors.reshape(tokens, heads, 2, 2, freqs)
    first = viewed[..., 0, :]
    second = viewed[..., 1, :]
    turned = jnp.stack([first * cosine - second * sine, first * sine + second * cosine], axis=-2)
    return turned.reshape(tokens, heads, width)


def spread_hidden(token_count, hidden_columns):
    return 2 * token_count < 3 * hidden_columns


def swap_blocks(blocks, split_axis):
    size = lax.axis_size("sp")
    here = lax.axis_index("sp")
    grp_size = lax.axis_size("grp")
    part = lax.axis_index("grp")
    half = blocks.shape[1] // grp_size
    mine = lax.dynamic_slice_in_dim(blocks, part * half, half, 1)
    arrived = []
    for shift in range(1, size):
        sent = lax.dynamic_index_in_dim(mine, (here + shift) % size, 0, keepdims=False)
        arrived.append(
            lax.ppermute(sent, "sp", [(i, (i + shift) % size) for i in range(size)])
        )
    own = lax.dynamic_index_in_dim(blocks, here, 0, keepdims=False)
    whole = jnp.zeros((size,) + blocks.shape[1:], blocks.dtype)
    whole = lax.dynamic_update_index_in_dim(whole, own, here, 0)
    for shift, piece in zip(range(1, size), arrived):
        origin = (here - shift + size) % size
        for turn in range(grp_size):
            got = piece
            if turn:
                got = lax.ppermute(
                    piece, "grp", [(i, (i + turn) % grp_size) for i in range(grp_size)]
                )
            owner = (part - turn + grp_size) % grp_size
            whole = lax.dynamic_update_slice(
                whole, got[None], (origin, owner * half) + (0,) * (blocks.ndim - 2)
            )
    return whole


def exchange_weights(gate_weight, up_weight, down_weight):
    size = lax.axis_size("sp")
    depth, columns = gate_weight.shape
    piece = columns // size
    split = lambda w: w.reshape(depth, size, piece)
    both = jnp.concatenate([split(gate_weight), split(up_weight)], axis=2)
    gate_up = swap_blocks(both.transpose(1, 0, 2), 1).reshape(size * depth, 2 * piece)
    down = swap_blocks(down_weight.reshape(size, piece, down_weight.shape[1]), 1)
    return gate_up, down


def spread_ffn(projected, residual, ffn_gain, gate_up, down):
    own_rows = residual.shape[0] // lax.axis_size("tp")
    tp_index = lax.axis_index("tp")
    summed = lax.psum_scatter(projected, "tp", scatter_dimension=0, tiled=True)
    residual_own = lax.dynamic_slice_in_dim(residual, tp_index * own_rows, own_rows, 0)
    mixed_own = residual_own.astype(jnp.float32) + summed.astype(jnp.float32)
    normed_own = norm_rows(mixed_own, ffn_gain).astype(jnp.bfloat16)
    normed = lax.all_gather(normed_own, ("sp", "tp"), axis=0, tiled=True)
    both = jnp.dot(normed, gate_up, preferred_element_type=jnp.float32)
    piece = gate_up.shape[1] // 2
    hidden = (jax.nn.silu(both[:, :piece]) * both[:, piece:]).astype(jnp.bfloat16)
    down_wide = down.transpose(1, 0, 2).reshape(piece, -1)
    terms = jnp.dot(hidden, down_wide, preferred_element_type=jnp.float32).astype(jnp.bfloat16)
    ffn_own = lax.psum_scatter(terms, ("sp", "tp"), scatter_dimension=0, tiled=True)
    return (mixed_own + ffn_own.astype(jnp.float32)).astype(jnp.bfloat16)


def local(
    query_nope,
    query_rope,
    token_latent,
    key_rope,
    latent_norm_gain,
    key_expand_weight,
    value_expand_weight,
    residual,
    out_weight,
    ffn_gain,
    gate_weight,
    up_weight,
    down_weight,
):
    sp_size = lax.axis_size("sp")
    spread = spread_hidden(query_nope.shape[0] * sp_size, gate_weight.shape[1])
    if spread:
        gate_up_own, down_own = exchange_weights(gate_weight, up_weight, down_weight)
    tok_rows = query_nope.shape[0]
    heads_here = query_nope.shape[1] // UNROTATED_SIZE
    own_rows = tok_rows // lax.axis_size("tp")
    tp_index = lax.axis_index("tp")
    positions = lax.axis_index("sp") * tok_rows + jnp.arange(tok_rows, dtype=jnp.int32)
    query_flat = query_nope.reshape(tok_rows, heads_here, UNROTATED_SIZE)
    query_turned = turn_heads(
        query_rope.astype(jnp.float32).reshape(tok_rows, heads_here, ROPE), positions
    ).astype(jnp.bfloat16)
    latent = norm_rows(token_latent, latent_norm_gain).astype(jnp.bfloat16)
    key_turned = turn_heads(key_rope.astype(jnp.float32)[:, None, :], positions)[:, 0].astype(
        jnp.bfloat16
    )
    key_cols = lax.dynamic_slice_in_dim(
        key_expand_weight, tp_index * heads_here * UNROTATED_SIZE, heads_here * UNROTATED_SIZE, 1
    )
    value_cols = lax.dynamic_slice_in_dim(
        value_expand_weight, tp_index * heads_here * VALUE_SIZE, heads_here * VALUE_SIZE, 1
    )
    score_scale = (UNROTATED_SIZE + ROPE) ** (-0.5)

    def absorb(carried, block_in):
        latent_block, rope_block = block_in
        block_rows = latent_block.shape[0]
        key_rows = jnp.dot(latent_block, key_cols, preferred_element_type=jnp.float32).astype(
            jnp.bfloat16
        )
        key_rows = key_rows.reshape(block_rows, heads_here, UNROTATED_SIZE)
        value_rows = jnp.dot(latent_block, value_cols, preferred_element_type=jnp.float32).astype(
            jnp.bfloat16
        )
        value_rows = value_rows.reshape(block_rows, heads_here, VALUE_SIZE)
        scores = (
            jnp.einsum("qhd,khd->hqk", query_flat, key_rows, preferred_element_type=jnp.float32)
            + jnp.einsum(
                "qhd,kd->hqk", query_turned, rope_block, preferred_element_type=jnp.float32
            )
        ) * score_scale
        highest, totals, accumulated = carried
        new_highest = jnp.maximum(highest, jnp.max(scores, axis=-1))
        shrink = jnp.exp(highest - new_highest)
        weights = jnp.exp(scores - new_highest[:, :, None])
        totals = totals * shrink + jnp.sum(weights, axis=-1)
        accumulated = accumulated * shrink.T[:, :, None] + jnp.einsum(
            "hqk,khd->qhd",
            weights.astype(jnp.bfloat16),
            value_rows,
            preferred_element_type=jnp.float32,
        )
        return ((new_highest, totals, accumulated), None)

    initial = (
        jnp.full((heads_here, tok_rows), -jnp.inf, jnp.float32),
        jnp.zeros((heads_here, tok_rows), jnp.float32),
        jnp.zeros((tok_rows, heads_here, VALUE_SIZE), jnp.float32),
    )
    carried = initial
    latent_piece = lax.all_gather(latent, "sp", axis=0, tiled=True)
    rope_piece = lax.all_gather(key_turned, "sp", axis=0, tiled=True)
    shard_count = latent_piece.shape[0] // tok_rows
    grouped = max(
        (
            factor
            for factor in range(1, shard_count + 1)
            if shard_count % factor == 0 and factor * tok_rows <= max(1024, tok_rows)
        )
    )
    block_rows = grouped * tok_rows
    blocks = (
        latent_piece.reshape(-1, block_rows, latent_piece.shape[1]),
        rope_piece.reshape(-1, block_rows, rope_piece.shape[1]),
    )
    carried, _ = lax.scan(absorb, carried, blocks)
    highest, totals, accumulated = carried
    attended = (
        (accumulated / totals.T[:, :, None])
        .reshape(tok_rows, heads_here * VALUE_SIZE)
        .astype(jnp.bfloat16)
    )
    projected = jnp.dot(attended, out_weight, preferred_element_type=jnp.float32).astype(
        jnp.bfloat16
    )
    if spread:
        return spread_ffn(projected, residual, ffn_gain, gate_up_own, down_own)
    summed = lax.psum(projected, "tp").astype(jnp.float32)
    mixed_all = residual.astype(jnp.float32) + summed
    normed_all = norm_rows(mixed_all, ffn_gain).astype(jnp.bfloat16)
    mixed_own = lax.dynamic_slice_in_dim(mixed_all, tp_index * own_rows, own_rows, 0)
    gate_piece = lax.all_gather(gate_weight, "sp", axis=0, tiled=True)
    up_piece = lax.all_gather(up_weight, "sp", axis=0, tiled=True)
    gate = jnp.dot(normed_all, gate_piece, preferred_element_type=jnp.float32)
    up_part = jnp.dot(normed_all, up_piece, preferred_element_type=jnp.float32)
    hidden = (jax.nn.silu(gate) * up_part).astype(jnp.bfloat16)
    terms = jnp.dot(
        hidden,
        lax.all_gather(down_weight, "sp", axis=1, tiled=True),
        preferred_element_type=jnp.float32,
    )
    ffn_own = lax.psum_scatter(
        terms.astype(jnp.bfloat16), "tp", scatter_dimension=0, tiled=True
    ).astype(jnp.float32)
    return (mixed_own + ffn_own).astype(jnp.bfloat16)


def solution(mesh):
    return jax.shard_map(
        local,
        mesh=mesh,
        in_specs=(
            P(("grp", "sp"), "tp"),
            P(("grp", "sp"), "tp"),
            P(("grp", "sp"), None),
            P(("grp", "sp"), None),
            P(),
            P(),
            P(),
            P(("grp", "sp"), None),
            P("tp", None),
            P(),
            P("sp", "tp"),
            P("sp", "tp"),
            P("tp", "sp"),
        ),
        out_specs=P(("grp", "sp", "tp"), None),
        check_vma=False,
    )
```

```python
import functools

import jax
import jax.numpy as jnp
from jax import lax
from jax.experimental import pallas as pl
from jax.experimental.pallas import tpu as pltpu
from jax.sharding import PartitionSpec as P

MESH = pl.DeviceIdType.MESH
UNROTATED_SIZE = 64
ROPE = 32
VALUE_SIZE = 64
GRID_W = 64


def norm_rows(values, gain):
    wide = values.astype(jnp.float32)
    return wide * lax.rsqrt(jnp.mean(wide * wide, axis=-1, keepdims=True) + 1e-06) * gain


def turn_heads(vectors, positions):
    tokens, heads, width = vectors.shape
    freqs = width // 4
    grid_pos = jnp.stack([positions // GRID_W, positions % GRID_W], axis=-1).astype(jnp.float32)
    inverse = jnp.power(10000.0, -jnp.arange(freqs, dtype=jnp.float32) / freqs)
    angles = grid_pos[:, :, None] * inverse
    cosine = jnp.cos(angles)[:, None]
    sine = jnp.sin(angles)[:, None]
    viewed = vectors.reshape(tokens, heads, 2, 2, freqs)
    first = viewed[..., 0, :]
    second = viewed[..., 1, :]
    turned = jnp.stack([first * cosine - second * sine, first * sine + second * cosine], axis=-2)
    return turned.reshape(tokens, heads, width)


def spread_hidden(token_count, hidden_columns):
    fits = lax.axis_size("tp") == 4 and lax.axis_size("grp") == 2
    return fits and 2 * token_count < 3 * hidden_columns


def column_tiles(hidden_columns):
    tiles = hidden_columns // 128
    return tiles, -(-tiles // lax.axis_size("sp"))


def window_start(at, hidden_columns):
    tiles, per = column_tiles(hidden_columns)
    return lax.div(at * (tiles - per), lax.axis_size("sp") - 1)


def signal_all(peers):
    barrier = pltpu.get_barrier_semaphore()
    for peer in peers:
        pl.semaphore_signal(barrier, inc=1, device_id=peer, device_id_type=MESH)
    pl.semaphore_wait(barrier, len(peers))


def remote(src, dst, send_sem, recv_sem, peer):
    return pltpu.make_async_remote_copy(
        src_ref=src,
        dst_ref=dst,
        send_sem=send_sem,
        recv_sem=recv_sem,
        device_id=peer,
        device_id_type=MESH,
    )


def weights_kernel(
    size, hidden_columns, gate, up, down, gate_out, up_out, down_out,
    own_sem, z_send, z_recv, y_send, y_recv,
):
    here = lax.axis_index("sp")
    part = lax.axis_index("grp")
    depth = gate.shape[0]
    width = gate_out.shape[1]
    outer = down.shape[1]

    def start_of(at):
        return pl.multiple_of(window_start(at, hidden_columns) * 128, 128)

    def piece(out, kind, origin, half):
        if kind < 2:
            rows = depth // 2
            return out.at[pl.ds(pl.multiple_of(origin * depth + half * rows, rows), rows), :]
        rows = width // 2
        return out.at[
            pl.ds(pl.multiple_of(half * rows, rows), rows),
            pl.ds(pl.multiple_of(origin * outer, outer), outer),
        ]

    def source(ref, kind, target, half):
        if kind < 2:
            rows = depth // 2
            return ref.at[pl.ds(pl.multiple_of(half * rows, rows), rows), pl.ds(start_of(target), width)]
        rows = width // 2
        return ref.at[pl.ds(pl.multiple_of(start_of(target) + half * rows, 64), rows), :]

    peers = [{"sp": lax.rem(here + shift, size)} for shift in range(1, size)]
    signal_all(peers + [{"grp": 1 - part}])
    refs = ((gate, gate_out), (up, up_out), (down, down_out))
    across = []
    for kind, (ref, out) in enumerate(refs):
        for shift in range(1, size):
            target = lax.rem(here + shift, size)
            copy = remote(
                source(ref, kind, target, part),
                piece(out, kind, here, part),
                z_send.at[kind, shift - 1],
                z_recv.at[kind, shift - 1],
                {"sp": target},
            )
            copy.start()
            across.append(copy)
    locals_ = []
    for kind, (ref, out) in enumerate(refs):
        for half in range(2):
            copy = pltpu.make_async_copy(
                source(ref, kind, here, half), piece(out, kind, here, half), own_sem.at[kind, half]
            )
            copy.start()
            locals_.append(copy)
    swaps = []
    for kind, (ref, out) in enumerate(refs):
        for shift in range(1, size):
            origin = lax.rem(here - shift + size, size)
            across[kind * (size - 1) + shift - 1].wait_recv()
            held = piece(out, kind, origin, part)
            copy = remote(
                held, held, y_send.at[kind, shift - 1], y_recv.at[kind, shift - 1], {"grp": 1 - part}
            )
            copy.start()
            swaps.append(copy)
    for copy in across:
        copy.wait_send()
    for copy in locals_:
        copy.wait()
    for copy in swaps:
        copy.wait()


def exchange_weights(gate_weight, up_weight, down_weight):
    size = lax.axis_size("sp")
    depth, columns = gate_weight.shape
    width = column_tiles(columns)[1] * 128
    wide = jax.ShapeDtypeStruct((size * depth, width), gate_weight.dtype)
    tall = jax.ShapeDtypeStruct((width, size * down_weight.shape[1]), down_weight.dtype)
    pairs = pltpu.SemaphoreType.DMA((3, size - 1))
    return pl.pallas_call(
        functools.partial(weights_kernel, size, columns),
        out_shape=(wide, wide, tall),
        in_specs=[pl.BlockSpec(memory_space=pl.ANY)] * 3,
        out_specs=[pl.BlockSpec(memory_space=pl.ANY)] * 3,
        scratch_shapes=[pltpu.SemaphoreType.DMA((3, 2)), pairs, pairs, pairs, pairs],
        compiler_params=pltpu.CompilerParams(collective_id=0, has_side_effects=True),
        name="swap_weights",
    )(gate_weight, up_weight, down_weight)


def ffn_kernel(
    size, own, gate_w, up_w, down_w, keep, mixed, out,
    tokens, parts, from_core, from_x, from_z, total,
    z_send, z_recv, x_send, x_recv, c_send, c_recv,
    rc_send, rc_recv, rx_send, rx_recv, rz_send, rz_recv,
):
    here = lax.axis_index("sp")
    t = lax.axis_index("tp")
    core = t + 1 - 2 * lax.rem(t, 2)
    across = t + 2 - 4 * lax.div(t, 2)
    diagonal = core + 2 - 4 * lax.div(core, 2)
    rows = own.shape[0]
    to_core, to_x = {"tp": core}, {"tp": across}
    signal_all(
        [{"sp": lax.rem(here + shift, size)} for shift in range(1, size)] + [to_core, to_x]
    )
    z_copies = [None]
    for shift in range(1, size):
        copy = remote(
            own,
            tokens.at[here, t],
            z_send.at[shift],
            z_recv.at[shift],
            {"sp": lax.rem(here + shift, size)},
        )
        copy.start()
        z_copies.append(copy)
    tokens[here, t] = own[...]
    origins = [lax.rem(here - i + size, size) for i in range(size)]
    pending = []
    x_copies, c_first, c_second, r_first, r_second, rx, rz = {}, {}, {}, {}, {}, {}, {}

    def start(table, i, *args):
        copy = remote(*args)
        copy.start()
        table[i] = copy
        pending.append(copy)

    def step_a(i):
        o = origins[i]
        if i:
            z_copies[i].wait_recv()
        block = tokens.at[o, t] if i else own
        start(x_copies, i, block, tokens.at[o, t], x_send.at[i], x_recv.at[i], to_x)
        start(c_first, i, block, tokens.at[o, t], c_send.at[i, 0], c_recv.at[i, 0], to_core)

    def step_b(i):
        o = origins[i]
        x_copies[i].wait_recv()
        block = tokens.at[o, across]
        start(c_second, i, block, block, c_send.at[i, 1], c_recv.at[i, 1], to_core)

    def step_c(i):
        o = origins[i]
        c_first[i].wait_recv()
        c_second[i].wait_recv()
        x = tokens[o].reshape(4 * rows, own.shape[1])
        gate = jnp.dot(x, gate_w[...], preferred_element_type=jnp.float32)
        up = jnp.dot(x, up_w[...], preferred_element_type=jnp.float32)
        hidden = (gate / (1.0 + jnp.exp(-gate)) * up * keep[...]).astype(jnp.bfloat16)
        step = 512
        for col in range(0, own.shape[1], step):
            term = jnp.dot(
                hidden, down_w[:, col : col + step], preferred_element_type=jnp.float32
            )
            parts[o, :, :, col : col + step] = term.astype(jnp.bfloat16).reshape(4, rows, step)
        start(r_first, i, parts.at[o, diagonal], from_core.at[i, 1], rc_send.at[i, 1], rc_recv.at[i, 1], to_core)
        start(r_second, i, parts.at[o, core], from_core.at[i, 0], rc_send.at[i, 0], rc_recv.at[i, 0], to_core)

    def plus(one, two):
        return one.astype(jnp.float32) + two.astype(jnp.float32)

    def step_d(i):
        o = origins[i]
        r_first[i].wait_recv()
        parts[o, across] = plus(parts[o, across], from_core[i, 1]).astype(jnp.bfloat16)
        start(rx, i, parts.at[o, across], from_x.at[i], rx_send.at[i], rx_recv.at[i], to_x)
        r_second[i].wait_recv()
        parts[o, t] = plus(parts[o, t], from_core[i, 0]).astype(jnp.bfloat16)

    def step_e(i):
        o = origins[i]
        rx[i].wait_recv()
        if i == 0:
            total[...] = mixed[...] + plus(parts[o, t], from_x[i])
            return
        parts[o, t] = plus(parts[o, t], from_x[i]).astype(jnp.bfloat16)
        start(rz, i, parts.at[o, t], from_z.at[i], rz_send.at[i], rz_recv.at[i], {"sp": o})

    steps = {"a": step_a, "b": step_b, "c": step_c, "d": step_d, "e": step_e}
    last = size - 1
    order = [("a", 0)]
    for i in range(size + 2):
        for name, lag in (("a", -1), ("b", 0), ("c", 0), ("d", 1), ("e", 2)):
            if 0 <= i - lag <= last:
                order.append((name, i - lag))
    for name, i in order:
        steps[name](i)
    result = total[...]
    for i in range(1, size):
        rz[i].wait_recv()
        result = result + from_z[i].astype(jnp.float32)
    out[...] = result.astype(out.dtype)
    for copy in z_copies[1:] + pending:
        copy.wait_send()


def spread_ffn(projected, residual, ffn_gain, swapped, hidden_columns):
    size = lax.axis_size("sp")
    own_rows = residual.shape[0] // lax.axis_size("tp")
    tp_index = lax.axis_index("tp")
    summed = lax.psum_scatter(projected, "tp", scatter_dimension=0, tiled=True)
    residual_own = lax.dynamic_slice_in_dim(residual, tp_index * own_rows, own_rows, 0)
    mixed_own = residual_own.astype(jnp.float32) + summed.astype(jnp.float32)
    normed_own = norm_rows(mixed_own, ffn_gain).astype(jnp.bfloat16)
    here = lax.axis_index("sp")
    per = column_tiles(hidden_columns)[1]
    before = jnp.where(here > 0, window_start(jnp.maximum(here - 1, 0), hidden_columns) + per, 0)
    first = (before - window_start(here, hidden_columns)) * 128
    keep = (jnp.arange(per * 128, dtype=jnp.int32) >= first).astype(jnp.float32)[None]
    width = residual.shape[1]
    block = (own_rows, width)
    dma = pltpu.SemaphoreType.DMA
    vmem = lambda *lead: pltpu.VMEM(lead + block, jnp.bfloat16)
    pair = [dma((size,)), dma((size,))]
    double = [dma((size, 2)), dma((size, 2))]
    return pl.pallas_call(
        functools.partial(ffn_kernel, size),
        out_shape=jax.ShapeDtypeStruct(block, jnp.bfloat16),
        in_specs=[pl.BlockSpec(memory_space=pltpu.VMEM)] * 6,
        out_specs=pl.BlockSpec(memory_space=pltpu.VMEM),
        scratch_shapes=[
            vmem(size, 4), vmem(size, 4), vmem(size, 2), vmem(size), vmem(size),
            pltpu.VMEM(block, jnp.float32),
        ] + pair + pair + double + double + pair + pair,
        compiler_params=pltpu.CompilerParams(collective_id=1, has_side_effects=True),
        name="spread_ffn",
    )(normed_own, *swapped, keep, mixed_own)


def local(
    query_nope,
    query_rope,
    token_latent,
    key_rope,
    latent_norm_gain,
    key_expand_weight,
    value_expand_weight,
    residual,
    out_weight,
    ffn_gain,
    gate_weight,
    up_weight,
    down_weight,
):
    sp_size = lax.axis_size("sp")
    spread = spread_hidden(query_nope.shape[0] * sp_size, gate_weight.shape[1])
    if spread:
        swapped = exchange_weights(gate_weight, up_weight, down_weight)
    tok_rows = query_nope.shape[0]
    heads_here = query_nope.shape[1] // UNROTATED_SIZE
    own_rows = tok_rows // lax.axis_size("tp")
    tp_index = lax.axis_index("tp")
    positions = lax.axis_index("sp") * tok_rows + jnp.arange(tok_rows, dtype=jnp.int32)
    query_flat = query_nope.reshape(tok_rows, heads_here, UNROTATED_SIZE)
    query_turned = turn_heads(
        query_rope.astype(jnp.float32).reshape(tok_rows, heads_here, ROPE), positions
    ).astype(jnp.bfloat16)
    latent = norm_rows(token_latent, latent_norm_gain).astype(jnp.bfloat16)
    key_turned = turn_heads(key_rope.astype(jnp.float32)[:, None, :], positions)[:, 0].astype(
        jnp.bfloat16
    )
    key_cols = lax.dynamic_slice_in_dim(
        key_expand_weight, tp_index * heads_here * UNROTATED_SIZE, heads_here * UNROTATED_SIZE, 1
    )
    value_cols = lax.dynamic_slice_in_dim(
        value_expand_weight, tp_index * heads_here * VALUE_SIZE, heads_here * VALUE_SIZE, 1
    )
    score_scale = (UNROTATED_SIZE + ROPE) ** (-0.5)

    def absorb(carried, block_in):
        latent_block, rope_block = block_in
        block_rows = latent_block.shape[0]
        key_rows = jnp.dot(latent_block, key_cols, preferred_element_type=jnp.float32).astype(
            jnp.bfloat16
        )
        key_rows = key_rows.reshape(block_rows, heads_here, UNROTATED_SIZE)
        value_rows = jnp.dot(latent_block, value_cols, preferred_element_type=jnp.float32).astype(
            jnp.bfloat16
        )
        value_rows = value_rows.reshape(block_rows, heads_here, VALUE_SIZE)
        scores = (
            jnp.einsum("qhd,khd->hqk", query_flat, key_rows, preferred_element_type=jnp.float32)
            + jnp.einsum(
                "qhd,kd->hqk", query_turned, rope_block, preferred_element_type=jnp.float32
            )
        ) * score_scale
        highest, totals, accumulated = carried
        new_highest = jnp.maximum(highest, jnp.max(scores, axis=-1))
        shrink = jnp.exp(highest - new_highest)
        weights = jnp.exp(scores - new_highest[:, :, None])
        totals = totals * shrink + jnp.sum(weights, axis=-1)
        accumulated = accumulated * shrink.T[:, :, None] + jnp.einsum(
            "hqk,khd->qhd",
            weights.astype(jnp.bfloat16),
            value_rows,
            preferred_element_type=jnp.float32,
        )
        return ((new_highest, totals, accumulated), None)

    initial = (
        jnp.full((heads_here, tok_rows), -jnp.inf, jnp.float32),
        jnp.zeros((heads_here, tok_rows), jnp.float32),
        jnp.zeros((tok_rows, heads_here, VALUE_SIZE), jnp.float32),
    )
    carried = initial
    latent_piece = lax.all_gather(latent, "sp", axis=0, tiled=True)
    rope_piece = lax.all_gather(key_turned, "sp", axis=0, tiled=True)
    shard_count = latent_piece.shape[0] // tok_rows
    grouped = max(
        (
            factor
            for factor in range(1, shard_count + 1)
            if shard_count % factor == 0 and factor * tok_rows <= max(1024, tok_rows)
        )
    )
    block_rows = grouped * tok_rows
    blocks = (
        latent_piece.reshape(-1, block_rows, latent_piece.shape[1]),
        rope_piece.reshape(-1, block_rows, rope_piece.shape[1]),
    )
    carried, _ = lax.scan(absorb, carried, blocks)
    highest, totals, accumulated = carried
    attended = (
        (accumulated / totals.T[:, :, None])
        .reshape(tok_rows, heads_here * VALUE_SIZE)
        .astype(jnp.bfloat16)
    )
    projected = jnp.dot(attended, out_weight, preferred_element_type=jnp.float32).astype(
        jnp.bfloat16
    )
    if spread:
        return spread_ffn(projected, residual, ffn_gain, swapped, gate_weight.shape[1])
    summed = lax.psum(projected, "tp").astype(jnp.float32)
    mixed_all = residual.astype(jnp.float32) + summed
    normed_all = norm_rows(mixed_all, ffn_gain).astype(jnp.bfloat16)
    mixed_own = lax.dynamic_slice_in_dim(mixed_all, tp_index * own_rows, own_rows, 0)
    gate_piece = lax.all_gather(gate_weight, "sp", axis=0, tiled=True)
    up_piece = lax.all_gather(up_weight, "sp", axis=0, tiled=True)
    gate = jnp.dot(normed_all, gate_piece, preferred_element_type=jnp.float32)
    up_part = jnp.dot(normed_all, up_piece, preferred_element_type=jnp.float32)
    hidden = (jax.nn.silu(gate) * up_part).astype(jnp.bfloat16)
    terms = jnp.dot(
        hidden,
        lax.all_gather(down_weight, "sp", axis=1, tiled=True),
        preferred_element_type=jnp.float32,
    )
    ffn_own = lax.psum_scatter(
        terms.astype(jnp.bfloat16), "tp", scatter_dimension=0, tiled=True
    ).astype(jnp.float32)
    return (mixed_own + ffn_own).astype(jnp.bfloat16)


def solution(mesh):
    return jax.shard_map(
        local,
        mesh=mesh,
        in_specs=(
            P(("grp", "sp"), "tp"),
            P(("grp", "sp"), "tp"),
            P(("grp", "sp"), None),
            P(("grp", "sp"), None),
            P(),
            P(),
            P(),
            P(("grp", "sp"), None),
            P("tp", None),
            P(),
            P("sp", "tp"),
            P("sp", "tp"),
            P("tp", "sp"),
        ),
        out_specs=P(("grp", "sp", "tp"), None),
        check_vma=False,
    )
```

```python
import functools

import jax
import jax.numpy as jnp
from jax import lax
from jax.experimental import pallas as pl
from jax.experimental.pallas import tpu as pltpu
from jax.sharding import PartitionSpec as P

MESH = pl.DeviceIdType.MESH
UNROTATED_SIZE = 64
ROPE = 32
VALUE_SIZE = 64
GRID_W = 64


def norm_rows(values, gain):
    wide = values.astype(jnp.float32)
    return wide * lax.rsqrt(jnp.mean(wide * wide, axis=-1, keepdims=True) + 1e-06) * gain


def turn_heads(vectors, positions):
    tokens, heads, width = vectors.shape
    freqs = width // 4
    grid_pos = jnp.stack([positions // GRID_W, positions % GRID_W], axis=-1).astype(jnp.float32)
    inverse = jnp.power(10000.0, -jnp.arange(freqs, dtype=jnp.float32) / freqs)
    angles = grid_pos[:, :, None] * inverse
    cosine = jnp.cos(angles)[:, None]
    sine = jnp.sin(angles)[:, None]
    viewed = vectors.reshape(tokens, heads, 2, 2, freqs)
    first = viewed[..., 0, :]
    second = viewed[..., 1, :]
    turned = jnp.stack([first * cosine - second * sine, first * sine + second * cosine], axis=-2)
    return turned.reshape(tokens, heads, width)


def spread_hidden(token_count, hidden_columns):
    fits = lax.axis_size("tp") == 4 and lax.axis_size("grp") == 2
    return fits and 2 * token_count < 3 * hidden_columns


def column_tiles(hidden_columns):
    tiles = hidden_columns // 128
    return tiles, -(-tiles // lax.axis_size("sp"))


def window_start(at, hidden_columns):
    tiles, per = column_tiles(hidden_columns)
    return lax.div(at * (tiles - per), lax.axis_size("sp") - 1)


def signal_all(peers):
    barrier = pltpu.get_barrier_semaphore()
    for peer in peers:
        pl.semaphore_signal(barrier, inc=1, device_id=peer, device_id_type=MESH)
    pl.semaphore_wait(barrier, len(peers))


def remote(src, dst, send_sem, recv_sem, peer):
    return pltpu.make_async_remote_copy(
        src_ref=src,
        dst_ref=dst,
        send_sem=send_sem,
        recv_sem=recv_sem,
        device_id=peer,
        device_id_type=MESH,
    )


def front_kernel(
    size, hidden_columns, query, turned, latent, key_w, value_w, out_w, residual, gain,
    gate, up, down,
    gate_out, up_out, down_out, mixed, normed,
    gathered, projected, landed,
    own_sem, z_send, z_recv, y_send, y_recv, l_send, l_recv, m_send, m_recv, r_send, r_recv,
):
    here = lax.axis_index("sp")
    part = lax.axis_index("grp")
    t = lax.axis_index("tp")
    side = lax.rem(t, 2)
    core = t + 1 - 2 * side
    depth = gate.shape[0]
    width = gate_out.shape[1]
    outer = down.shape[1]

    def start_of(at):
        return pl.multiple_of(window_start(at, hidden_columns) * 128, 128)

    def piece(out, kind, origin, half):
        if kind < 2:
            rows = depth // 2
            return out.at[pl.ds(pl.multiple_of(origin * depth + half * rows, rows), rows), :]
        rows = width // 2
        return out.at[
            pl.ds(pl.multiple_of(half * rows, rows), rows),
            pl.ds(pl.multiple_of(origin * outer, outer), outer),
        ]

    def source(ref, kind, target, half):
        if kind < 2:
            rows = depth // 2
            return ref.at[pl.ds(pl.multiple_of(half * rows, rows), rows), pl.ds(start_of(target), width)]
        rows = width // 2
        return ref.at[pl.ds(pl.multiple_of(start_of(target) + half * rows, 64), rows), :]

    peers = [{"sp": lax.rem(here + shift, size)} for shift in range(1, size)]
    peers += [{"tp": lax.rem(t + shift, 4)} for shift in range(1, 4)]
    signal_all(peers + [{"grp": 1 - part}])
    tokens = latent.shape[0]
    half_rows = tokens // 2
    my_half = pl.ds(pl.multiple_of(side * half_rows, half_rows), half_rows)
    spread_latent = []
    for shift in range(1, size):
        copy = remote(
            latent.at[my_half, :],
            gathered.at[here, my_half, :],
            l_send.at[shift - 1],
            l_recv.at[shift - 1],
            {"sp": lax.rem(here + shift, size)},
        )
        copy.start()
        spread_latent.append(copy)
    refs = ((gate, gate_out), (up, up_out), (down, down_out))
    across = []
    for kind, (ref, out) in enumerate(refs):
        for shift in range(1, size):
            target = lax.rem(here + shift, size)
            copy = remote(
                source(ref, kind, target, part),
                piece(out, kind, here, part),
                z_send.at[kind, shift - 1],
                z_recv.at[kind, shift - 1],
                {"sp": target},
            )
            copy.start()
            across.append(copy)
    locals_ = []
    for kind, (ref, out) in enumerate(refs):
        for half in range(2):
            copy = pltpu.make_async_copy(
                source(ref, kind, here, half), piece(out, kind, here, half), own_sem.at[kind, half]
            )
            copy.start()
            locals_.append(copy)
    gathered[here] = latent[...]
    shared_latent = []
    for shift in range(1, size):
        spread_latent[shift - 1].wait_recv()
        held = gathered.at[lax.rem(here - shift + size, size), my_half, :]
        copy = remote(held, held, m_send.at[shift - 1], m_recv.at[shift - 1], {"tp": core})
        copy.start()
        shared_latent.append(copy)
    for copy in shared_latent:
        copy.wait_recv()

    lanes = query.shape[1]
    heads = lanes // UNROTATED_SIZE
    rank = key_w.shape[0]
    columns = pl.ds(pl.multiple_of(t * lanes, 128), lanes)
    every = gathered[...].reshape(size * tokens, latent.shape[1])
    every_latent = every[:, :rank]
    keys = jnp.dot(every_latent, key_w[:, columns], preferred_element_type=jnp.float32)
    values = jnp.dot(every_latent, value_w[:, columns], preferred_element_type=jnp.float32)
    values = values.astype(jnp.bfloat16)
    keys = jnp.concatenate([keys.astype(jnp.bfloat16), every[:, rank:]], axis=1)
    scale = (UNROTATED_SIZE + ROPE) ** (-0.5)
    lane = lax.broadcasted_iota(jnp.int32, (1, lanes), 1)
    rope_lane = lax.broadcasted_iota(jnp.int32, (1, turned.shape[1]), 1)
    attended = jnp.zeros((tokens, lanes), jnp.float32)
    for head in range(heads):
        mine = (lane >= head * UNROTATED_SIZE) & (lane < (head + 1) * UNROTATED_SIZE)
        rope_mine = (rope_lane >= head * ROPE) & (rope_lane < (head + 1) * ROPE)
        both = jnp.concatenate(
            [
                jnp.where(mine, query[...].astype(jnp.float32), 0.0),
                jnp.where(rope_mine, turned[...].astype(jnp.float32), 0.0),
            ],
            axis=1,
        ).astype(jnp.bfloat16)
        scores = (
            lax.dot_general(
                both, keys, (((1,), (1,)), ((), ())), preferred_element_type=jnp.float32
            )
            * scale
        )
        raised = jnp.exp(scores - jnp.max(scores, axis=1, keepdims=True))
        totals = jnp.sum(raised, axis=1, keepdims=True)
        weighted = jnp.dot(
            raised.astype(jnp.bfloat16), values, preferred_element_type=jnp.float32
        )
        attended = jnp.where(mine, weighted / totals, attended)
    attended = attended.astype(jnp.bfloat16)
    own_rows = mixed.shape[0]
    step = 512
    for col in range(0, out_w.shape[1], step):
        term = jnp.dot(
            attended, out_w[:, col : col + step], preferred_element_type=jnp.float32
        )
        projected[:, :, col : col + step] = term.astype(jnp.bfloat16).reshape(4, own_rows, step)
    scattered = []
    for shift in (2, 1, 3):
        target = lax.rem(t + shift, 4)
        copy = remote(
            projected.at[target],
            landed.at[shift - 1],
            r_send.at[shift - 1],
            r_recv.at[shift - 1],
            {"tp": target},
        )
        copy.start()
        scattered.append(copy)

    swaps = []

    def forward(kind):
        out = refs[kind][1]
        for shift in range(1, size):
            origin = lax.rem(here - shift + size, size)
            across[kind * (size - 1) + shift - 1].wait_recv()
            held = piece(out, kind, origin, part)
            copy = remote(
                held, held, y_send.at[kind, shift - 1], y_recv.at[kind, shift - 1], {"grp": 1 - part}
            )
            copy.start()
            swaps.append(copy)

    forward(0)
    forward(1)
    for copy in scattered:
        copy.wait_recv()
    rows = pl.ds(pl.multiple_of(t * own_rows, own_rows), own_rows)
    total = residual[rows, :].astype(jnp.float32) + projected[t].astype(jnp.float32)
    for shift in range(3):
        total = total + landed[shift].astype(jnp.float32)
    mixed[...] = total
    normed[...] = (
        total * lax.rsqrt(jnp.mean(total * total, axis=1, keepdims=True) + 1e-06) * gain[...]
    ).astype(jnp.bfloat16)
    forward(2)
    for copy in across + spread_latent + shared_latent + scattered:
        copy.wait_send()
    for copy in locals_:
        copy.wait()
    for copy in swaps:
        copy.wait()


def front(query, turned, latent, key_w, value_w, out_w, residual, gain, gate, up, down):
    size = lax.axis_size("sp")
    depth, columns = gate.shape
    width = column_tiles(columns)[1] * 128
    own = (residual.shape[0] // lax.axis_size("tp"), residual.shape[1])
    wide = jax.ShapeDtypeStruct((size * depth, width), gate.dtype)
    tall = jax.ShapeDtypeStruct((width, size * down.shape[1]), down.dtype)
    dma = pltpu.SemaphoreType.DMA
    pairs = dma((3, size - 1))
    line = dma((size - 1,))
    here = pl.BlockSpec(memory_space=pltpu.VMEM)
    away = pl.BlockSpec(memory_space=pl.ANY)
    return pl.pallas_call(
        functools.partial(front_kernel, size, columns),
        out_shape=(
            wide, wide, tall,
            jax.ShapeDtypeStruct(own, jnp.float32), jax.ShapeDtypeStruct(own, jnp.bfloat16),
        ),
        in_specs=[here] * 8 + [away] * 3,
        out_specs=[away] * 3 + [here] * 2,
        scratch_shapes=[
            pltpu.VMEM((size,) + latent.shape, jnp.bfloat16),
            pltpu.VMEM((4,) + own, jnp.bfloat16),
            pltpu.VMEM((3,) + own, jnp.bfloat16),
            dma((3, 2)), pairs, pairs, pairs, pairs, line, line, line, line, dma((3,)), dma((3,)),
        ],
        compiler_params=pltpu.CompilerParams(collective_id=0, has_side_effects=True),
        name="front",
    )(query, turned, latent, key_w, value_w, out_w, residual, gain, gate, up, down)


def turn_lanes(vectors, positions):
    lanes = vectors.shape[1]
    freqs = ROPE // 4
    lane = jnp.arange(lanes, dtype=jnp.int32)
    inverse = jnp.power(10000.0, -(lane % freqs).astype(jnp.float32) / freqs)
    first_axis = lane % ROPE < ROPE // 2
    first_half = lane % (2 * freqs) < freqs
    place = jnp.where(
        first_axis[None], (positions // GRID_W)[:, None], (positions % GRID_W)[:, None]
    )
    angles = place.astype(jnp.float32) * inverse[None]
    partner = jnp.where(first_half, lane + freqs, lane - freqs)
    sign = jnp.where(first_half, -1.0, 1.0)
    swap = jnp.where(lane[:, None] == partner[None], sign[None], 0.0).astype(vectors.dtype)
    other = jnp.dot(vectors, swap, preferred_element_type=jnp.float32)
    turned = vectors.astype(jnp.float32) * jnp.cos(angles) + other * jnp.sin(angles)
    return turned.astype(jnp.bfloat16)


def spread_layer(
    query_nope, query_rope, token_latent, key_rope, latent_norm_gain, key_w, value_w,
    residual, out_w, ffn_gain, gate_w, up_w, down_w,
):
    rows = query_nope.shape[0]
    positions = lax.axis_index("sp") * rows + jnp.arange(rows, dtype=jnp.int32)
    repeats = query_rope.shape[1] // ROPE
    turned = turn_lanes(query_rope, positions)
    key_turned = turn_lanes(jnp.tile(key_rope, (1, repeats)), positions)
    latent = norm_rows(token_latent, latent_norm_gain).astype(jnp.bfloat16)
    packed = jnp.concatenate([latent, key_turned], axis=1)
    gate, up, down, mixed, normed = front(
        query_nope, turned, packed, key_w, value_w, out_w, residual, ffn_gain[None],
        gate_w, up_w, down_w,
    )
    return spread_ffn(normed, mixed, (gate, up, down), gate_w.shape[1])


def ffn_kernel(
    size, own, gate_w, up_w, down_w, keep, mixed, out,
    tokens, parts, from_core, from_x, from_z, total,
    z_send, z_recv, x_send, x_recv, c_send, c_recv,
    rc_send, rc_recv, rx_send, rx_recv, rz_send, rz_recv,
):
    here = lax.axis_index("sp")
    t = lax.axis_index("tp")
    core = t + 1 - 2 * lax.rem(t, 2)
    across = t + 2 - 4 * lax.div(t, 2)
    diagonal = core + 2 - 4 * lax.div(core, 2)
    rows = own.shape[0]
    to_core, to_x = {"tp": core}, {"tp": across}
    signal_all(
        [{"sp": lax.rem(here + shift, size)} for shift in range(1, size)] + [to_core, to_x]
    )
    z_copies = [None]
    for shift in range(1, size):
        copy = remote(
            own,
            tokens.at[here, t],
            z_send.at[shift],
            z_recv.at[shift],
            {"sp": lax.rem(here + shift, size)},
        )
        copy.start()
        z_copies.append(copy)
    tokens[here, t] = own[...]
    origins = [lax.rem(here - i + size, size) for i in range(size)]
    pending = []
    x_copies, c_first, c_second, r_first, r_second, rx, rz = {}, {}, {}, {}, {}, {}, {}

    def start(table, i, *args):
        copy = remote(*args)
        copy.start()
        table[i] = copy
        pending.append(copy)

    def step_a(i):
        o = origins[i]
        if i:
            z_copies[i].wait_recv()
        block = tokens.at[o, t] if i else own
        start(x_copies, i, block, tokens.at[o, t], x_send.at[i], x_recv.at[i], to_x)
        start(c_first, i, block, tokens.at[o, t], c_send.at[i, 0], c_recv.at[i, 0], to_core)

    def step_b(i):
        o = origins[i]
        x_copies[i].wait_recv()
        block = tokens.at[o, across]
        start(c_second, i, block, block, c_send.at[i, 1], c_recv.at[i, 1], to_core)

    def step_c(i):
        o = origins[i]
        c_first[i].wait_recv()
        c_second[i].wait_recv()
        x = tokens[o].reshape(4 * rows, own.shape[1])
        gate = jnp.dot(x, gate_w[...], preferred_element_type=jnp.float32)
        up = jnp.dot(x, up_w[...], preferred_element_type=jnp.float32)
        hidden = (gate / (1.0 + jnp.exp(-gate)) * up * keep[...]).astype(jnp.bfloat16)
        step = 512
        for col in range(0, own.shape[1], step):
            term = jnp.dot(
                hidden, down_w[:, col : col + step], preferred_element_type=jnp.float32
            )
            parts[o, :, :, col : col + step] = term.astype(jnp.bfloat16).reshape(4, rows, step)
        start(r_first, i, parts.at[o, diagonal], from_core.at[i, 1], rc_send.at[i, 1], rc_recv.at[i, 1], to_core)
        start(r_second, i, parts.at[o, core], from_core.at[i, 0], rc_send.at[i, 0], rc_recv.at[i, 0], to_core)

    def plus(one, two):
        return one.astype(jnp.float32) + two.astype(jnp.float32)

    def step_d(i):
        o = origins[i]
        r_first[i].wait_recv()
        parts[o, across] = plus(parts[o, across], from_core[i, 1]).astype(jnp.bfloat16)
        start(rx, i, parts.at[o, across], from_x.at[i], rx_send.at[i], rx_recv.at[i], to_x)
        r_second[i].wait_recv()
        parts[o, t] = plus(parts[o, t], from_core[i, 0]).astype(jnp.bfloat16)

    def step_e(i):
        o = origins[i]
        rx[i].wait_recv()
        if i == 0:
            total[...] = mixed[...] + plus(parts[o, t], from_x[i])
            return
        parts[o, t] = plus(parts[o, t], from_x[i]).astype(jnp.bfloat16)
        start(rz, i, parts.at[o, t], from_z.at[i], rz_send.at[i], rz_recv.at[i], {"sp": o})

    steps = {"a": step_a, "b": step_b, "c": step_c, "d": step_d, "e": step_e}
    last = size - 1
    order = [("a", 0)]
    for i in range(size + 2):
        for name, lag in (("a", -1), ("b", 0), ("c", 0), ("d", 1), ("e", 2)):
            if 0 <= i - lag <= last:
                order.append((name, i - lag))
    for name, i in order:
        steps[name](i)
    result = total[...]
    for i in range(1, size):
        rz[i].wait_recv()
        result = result + from_z[i].astype(jnp.float32)
    out[...] = result.astype(out.dtype)
    for copy in z_copies[1:] + pending:
        copy.wait_send()


def spread_ffn(normed_own, mixed_own, swapped, hidden_columns):
    size = lax.axis_size("sp")
    here = lax.axis_index("sp")
    per = column_tiles(hidden_columns)[1]
    before = jnp.where(here > 0, window_start(jnp.maximum(here - 1, 0), hidden_columns) + per, 0)
    first = (before - window_start(here, hidden_columns)) * 128
    keep = (jnp.arange(per * 128, dtype=jnp.int32) >= first).astype(jnp.float32)[None]
    block = normed_own.shape
    dma = pltpu.SemaphoreType.DMA
    vmem = lambda *lead: pltpu.VMEM(lead + block, jnp.bfloat16)
    pair = [dma((size,)), dma((size,))]
    double = [dma((size, 2)), dma((size, 2))]
    return pl.pallas_call(
        functools.partial(ffn_kernel, size),
        out_shape=jax.ShapeDtypeStruct(block, jnp.bfloat16),
        in_specs=[pl.BlockSpec(memory_space=pltpu.VMEM)] * 6,
        out_specs=pl.BlockSpec(memory_space=pltpu.VMEM),
        scratch_shapes=[
            vmem(size, 4), vmem(size, 4), vmem(size, 2), vmem(size), vmem(size),
            pltpu.VMEM(block, jnp.float32),
        ] + pair + pair + double + double + pair + pair,
        compiler_params=pltpu.CompilerParams(collective_id=1, has_side_effects=True),
        name="spread_ffn",
    )(normed_own, *swapped, keep, mixed_own)


def local(
    query_nope,
    query_rope,
    token_latent,
    key_rope,
    latent_norm_gain,
    key_expand_weight,
    value_expand_weight,
    residual,
    out_weight,
    ffn_gain,
    gate_weight,
    up_weight,
    down_weight,
):
    if spread_hidden(query_nope.shape[0] * lax.axis_size("sp"), gate_weight.shape[1]):
        return spread_layer(
            query_nope,
            query_rope,
            token_latent,
            key_rope,
            latent_norm_gain,
            key_expand_weight,
            value_expand_weight,
            residual,
            out_weight,
            ffn_gain,
            gate_weight,
            up_weight,
            down_weight,
        )
    tok_rows = query_nope.shape[0]
    heads_here = query_nope.shape[1] // UNROTATED_SIZE
    own_rows = tok_rows // lax.axis_size("tp")
    tp_index = lax.axis_index("tp")
    positions = lax.axis_index("sp") * tok_rows + jnp.arange(tok_rows, dtype=jnp.int32)
    query_flat = query_nope.reshape(tok_rows, heads_here, UNROTATED_SIZE)
    query_turned = turn_heads(
        query_rope.astype(jnp.float32).reshape(tok_rows, heads_here, ROPE), positions
    ).astype(jnp.bfloat16)
    latent = norm_rows(token_latent, latent_norm_gain).astype(jnp.bfloat16)
    key_turned = turn_heads(key_rope.astype(jnp.float32)[:, None, :], positions)[:, 0].astype(
        jnp.bfloat16
    )
    key_cols = lax.dynamic_slice_in_dim(
        key_expand_weight, tp_index * heads_here * UNROTATED_SIZE, heads_here * UNROTATED_SIZE, 1
    )
    value_cols = lax.dynamic_slice_in_dim(
        value_expand_weight, tp_index * heads_here * VALUE_SIZE, heads_here * VALUE_SIZE, 1
    )
    score_scale = (UNROTATED_SIZE + ROPE) ** (-0.5)

    def absorb(carried, block_in):
        latent_block, rope_block = block_in
        block_rows = latent_block.shape[0]
        key_rows = jnp.dot(latent_block, key_cols, preferred_element_type=jnp.float32).astype(
            jnp.bfloat16
        )
        key_rows = key_rows.reshape(block_rows, heads_here, UNROTATED_SIZE)
        value_rows = jnp.dot(latent_block, value_cols, preferred_element_type=jnp.float32).astype(
            jnp.bfloat16
        )
        value_rows = value_rows.reshape(block_rows, heads_here, VALUE_SIZE)
        scores = (
            jnp.einsum("qhd,khd->hqk", query_flat, key_rows, preferred_element_type=jnp.float32)
            + jnp.einsum(
                "qhd,kd->hqk", query_turned, rope_block, preferred_element_type=jnp.float32
            )
        ) * score_scale
        highest, totals, accumulated = carried
        new_highest = jnp.maximum(highest, jnp.max(scores, axis=-1))
        shrink = jnp.exp(highest - new_highest)
        weights = jnp.exp(scores - new_highest[:, :, None])
        totals = totals * shrink + jnp.sum(weights, axis=-1)
        accumulated = accumulated * shrink.T[:, :, None] + jnp.einsum(
            "hqk,khd->qhd",
            weights.astype(jnp.bfloat16),
            value_rows,
            preferred_element_type=jnp.float32,
        )
        return ((new_highest, totals, accumulated), None)

    initial = (
        jnp.full((heads_here, tok_rows), -jnp.inf, jnp.float32),
        jnp.zeros((heads_here, tok_rows), jnp.float32),
        jnp.zeros((tok_rows, heads_here, VALUE_SIZE), jnp.float32),
    )
    carried = initial
    latent_piece = lax.all_gather(latent, "sp", axis=0, tiled=True)
    rope_piece = lax.all_gather(key_turned, "sp", axis=0, tiled=True)
    shard_count = latent_piece.shape[0] // tok_rows
    grouped = max(
        (
            factor
            for factor in range(1, shard_count + 1)
            if shard_count % factor == 0 and factor * tok_rows <= max(1024, tok_rows)
        )
    )
    block_rows = grouped * tok_rows
    blocks = (
        latent_piece.reshape(-1, block_rows, latent_piece.shape[1]),
        rope_piece.reshape(-1, block_rows, rope_piece.shape[1]),
    )
    carried, _ = lax.scan(absorb, carried, blocks)
    highest, totals, accumulated = carried
    attended = (
        (accumulated / totals.T[:, :, None])
        .reshape(tok_rows, heads_here * VALUE_SIZE)
        .astype(jnp.bfloat16)
    )
    projected = jnp.dot(attended, out_weight, preferred_element_type=jnp.float32).astype(
        jnp.bfloat16
    )
    summed = lax.psum(projected, "tp").astype(jnp.float32)
    mixed_all = residual.astype(jnp.float32) + summed
    normed_all = norm_rows(mixed_all, ffn_gain).astype(jnp.bfloat16)
    mixed_own = lax.dynamic_slice_in_dim(mixed_all, tp_index * own_rows, own_rows, 0)
    gate_piece = lax.all_gather(gate_weight, "sp", axis=0, tiled=True)
    up_piece = lax.all_gather(up_weight, "sp", axis=0, tiled=True)
    gate = jnp.dot(normed_all, gate_piece, preferred_element_type=jnp.float32)
    up_part = jnp.dot(normed_all, up_piece, preferred_element_type=jnp.float32)
    hidden = (jax.nn.silu(gate) * up_part).astype(jnp.bfloat16)
    terms = jnp.dot(
        hidden,
        lax.all_gather(down_weight, "sp", axis=1, tiled=True),
        preferred_element_type=jnp.float32,
    )
    ffn_own = lax.psum_scatter(
        terms.astype(jnp.bfloat16), "tp", scatter_dimension=0, tiled=True
    ).astype(jnp.float32)
    return (mixed_own + ffn_own).astype(jnp.bfloat16)


def solution(mesh):
    return jax.shard_map(
        local,
        mesh=mesh,
        in_specs=(
            P(("grp", "sp"), "tp"),
            P(("grp", "sp"), "tp"),
            P(("grp", "sp"), None),
            P(("grp", "sp"), None),
            P(),
            P(),
            P(),
            P(("grp", "sp"), None),
            P("tp", None),
            P(),
            P("sp", "tp"),
            P("sp", "tp"),
            P("tp", "sp"),
        ),
        out_specs=P(("grp", "sp", "tp"), None),
        check_vma=False,
    )
```

```python
import functools

import jax
import jax.numpy as jnp
from jax import lax
from jax.experimental import pallas as pl
from jax.experimental.pallas import tpu as pltpu
from jax.sharding import PartitionSpec as P

MESH = pl.DeviceIdType.MESH
UNROTATED_SIZE = 64
ROPE = 32
VALUE_SIZE = 64
GRID_W = 64


def norm_rows(values, gain):
    wide = values.astype(jnp.float32)
    return wide * lax.rsqrt(jnp.mean(wide * wide, axis=-1, keepdims=True) + 1e-06) * gain


def turn_heads(vectors, positions):
    tokens, heads, width = vectors.shape
    freqs = width // 4
    grid_pos = jnp.stack([positions // GRID_W, positions % GRID_W], axis=-1).astype(jnp.float32)
    inverse = jnp.power(10000.0, -jnp.arange(freqs, dtype=jnp.float32) / freqs)
    angles = grid_pos[:, :, None] * inverse
    cosine = jnp.cos(angles)[:, None]
    sine = jnp.sin(angles)[:, None]
    viewed = vectors.reshape(tokens, heads, 2, 2, freqs)
    first = viewed[..., 0, :]
    second = viewed[..., 1, :]
    turned = jnp.stack([first * cosine - second * sine, first * sine + second * cosine], axis=-2)
    return turned.reshape(tokens, heads, width)


def spread_hidden(token_count, hidden_columns):
    fits = lax.axis_size("tp") == 4 and lax.axis_size("grp") == 2
    return fits and 2 * token_count < 3 * hidden_columns


def column_tiles(hidden_columns):
    tiles = hidden_columns // 128
    return tiles, -(-tiles // lax.axis_size("sp"))


def window_start(at, hidden_columns):
    tiles, per = column_tiles(hidden_columns)
    return lax.div(at * (tiles - per), lax.axis_size("sp") - 1)


def signal_all(peers):
    barrier = pltpu.get_barrier_semaphore()
    for peer in peers:
        pl.semaphore_signal(barrier, inc=1, device_id=peer, device_id_type=MESH)
    pl.semaphore_wait(barrier, len(peers))


def remote(src, dst, send_sem, recv_sem, peer):
    return pltpu.make_async_remote_copy(
        src_ref=src,
        dst_ref=dst,
        send_sem=send_sem,
        recv_sem=recv_sem,
        device_id=peer,
        device_id_type=MESH,
    )


def front_kernel(
    size, hidden_columns, query, turned, latent, key_w, value_w, out_w, residual, gain,
    gate, up, down,
    gate_out, up_out, down_out, mixed, normed,
    gathered, projected, landed,
    own_sem, z_send, z_recv, y_send, y_recv, l_send, l_recv, m_send, m_recv, r_send, r_recv,
):
    here = lax.axis_index("sp")
    part = lax.axis_index("grp")
    t = lax.axis_index("tp")
    side = lax.rem(t, 2)
    core = t + 1 - 2 * side
    depth = gate.shape[0]
    width = gate_out.shape[1]
    outer = down.shape[1]

    def start_of(at):
        return pl.multiple_of(window_start(at, hidden_columns) * 128, 128)

    def piece(out, kind, origin, half):
        if kind < 2:
            rows = depth // 2
            return out.at[pl.ds(pl.multiple_of(origin * depth + half * rows, rows), rows), :]
        rows = width // 2
        return out.at[
            pl.ds(pl.multiple_of(half * rows, rows), rows),
            pl.ds(pl.multiple_of(origin * outer, outer), outer),
        ]

    def source(ref, kind, target, half):
        if kind < 2:
            rows = depth // 2
            return ref.at[pl.ds(pl.multiple_of(half * rows, rows), rows), pl.ds(start_of(target), width)]
        rows = width // 2
        return ref.at[pl.ds(pl.multiple_of(start_of(target) + half * rows, 64), rows), :]

    peers = [{"sp": lax.rem(here + shift, size)} for shift in range(1, size)]
    peers += [{"tp": lax.rem(t + shift, 4)} for shift in range(1, 4)]
    signal_all(peers + [{"grp": 1 - part}])
    tokens = latent.shape[0]
    half_rows = tokens // 2
    my_half = pl.ds(pl.multiple_of(side * half_rows, half_rows), half_rows)
    spread_latent = []
    for shift in range(1, size):
        copy = remote(
            latent.at[my_half, :],
            gathered.at[here, my_half, :],
            l_send.at[shift - 1],
            l_recv.at[shift - 1],
            {"sp": lax.rem(here + shift, size)},
        )
        copy.start()
        spread_latent.append(copy)
    refs = ((gate, gate_out), (up, up_out), (down, down_out))
    across = []
    for kind, (ref, out) in enumerate(refs):
        for shift in range(1, size):
            target = lax.rem(here + shift, size)
            copy = remote(
                source(ref, kind, target, part),
                piece(out, kind, here, part),
                z_send.at[kind, shift - 1],
                z_recv.at[kind, shift - 1],
                {"sp": target},
            )
            copy.start()
            across.append(copy)
    locals_ = []
    for kind, (ref, out) in enumerate(refs):
        for half in range(2):
            copy = pltpu.make_async_copy(
                source(ref, kind, here, half), piece(out, kind, here, half), own_sem.at[kind, half]
            )
            copy.start()
            locals_.append(copy)
    gathered[here] = latent[...]
    shared_latent = []
    for shift in range(1, size):
        spread_latent[shift - 1].wait_recv()
        held = gathered.at[lax.rem(here - shift + size, size), my_half, :]
        copy = remote(held, held, m_send.at[shift - 1], m_recv.at[shift - 1], {"tp": core})
        copy.start()
        shared_latent.append(copy)
    for copy in shared_latent:
        copy.wait_recv()

    lanes = query.shape[1]
    heads = lanes // UNROTATED_SIZE
    rank = key_w.shape[0]
    columns = pl.ds(pl.multiple_of(t * lanes, 128), lanes)
    every = gathered[...].reshape(size * tokens, latent.shape[1])
    every_latent = every[:, :rank]
    keys = jnp.dot(every_latent, key_w[:, columns], preferred_element_type=jnp.float32)
    values = jnp.dot(every_latent, value_w[:, columns], preferred_element_type=jnp.float32)
    values = values.astype(jnp.bfloat16)
    keys = jnp.concatenate([keys.astype(jnp.bfloat16), every[:, rank:]], axis=1)
    scale = (UNROTATED_SIZE + ROPE) ** (-0.5)
    lane = lax.broadcasted_iota(jnp.int32, (1, lanes), 1)
    rope_lane = lax.broadcasted_iota(jnp.int32, (1, turned.shape[1]), 1)
    attended = jnp.zeros((tokens, lanes), jnp.float32)
    for head in range(heads):
        mine = (lane >= head * UNROTATED_SIZE) & (lane < (head + 1) * UNROTATED_SIZE)
        rope_mine = (rope_lane >= head * ROPE) & (rope_lane < (head + 1) * ROPE)
        both = jnp.concatenate(
            [
                jnp.where(mine, query[...].astype(jnp.float32), 0.0),
                jnp.where(rope_mine, turned[...].astype(jnp.float32), 0.0),
            ],
            axis=1,
        ).astype(jnp.bfloat16)
        scores = (
            lax.dot_general(
                both, keys, (((1,), (1,)), ((), ())), preferred_element_type=jnp.float32
            )
            * scale
        )
        raised = jnp.exp(scores - jnp.max(scores, axis=1, keepdims=True))
        totals = jnp.sum(raised, axis=1, keepdims=True)
        weighted = jnp.dot(
            raised.astype(jnp.bfloat16), values, preferred_element_type=jnp.float32
        )
        attended = jnp.where(mine, weighted / totals, attended)
    attended = attended.astype(jnp.bfloat16)
    own_rows = mixed.shape[0]
    step = 512
    for col in range(0, out_w.shape[1], step):
        term = jnp.dot(
            attended, out_w[:, col : col + step], preferred_element_type=jnp.float32
        )
        projected[:, :, col : col + step] = term.astype(jnp.bfloat16).reshape(4, own_rows, step)
    scattered = []
    for shift in (2, 1, 3):
        target = lax.rem(t + shift, 4)
        copy = remote(
            projected.at[target],
            landed.at[shift - 1],
            r_send.at[shift - 1],
            r_recv.at[shift - 1],
            {"tp": target},
        )
        copy.start()
        scattered.append(copy)

    swaps = []

    def forward(kind):
        out = refs[kind][1]
        for shift in range(1, size):
            origin = lax.rem(here - shift + size, size)
            across[kind * (size - 1) + shift - 1].wait_recv()
            held = piece(out, kind, origin, part)
            copy = remote(
                held, held, y_send.at[kind, shift - 1], y_recv.at[kind, shift - 1], {"grp": 1 - part}
            )
            copy.start()
            swaps.append(copy)

    forward(0)
    forward(1)
    for copy in scattered:
        copy.wait_recv()
    rows = pl.ds(pl.multiple_of(t * own_rows, own_rows), own_rows)
    total = residual[rows, :].astype(jnp.float32) + projected[t].astype(jnp.float32)
    for shift in range(3):
        total = total + landed[shift].astype(jnp.float32)
    mixed[...] = total
    normed[...] = (
        total * lax.rsqrt(jnp.mean(total * total, axis=1, keepdims=True) + 1e-06) * gain[...]
    ).astype(jnp.bfloat16)
    forward(2)
    for copy in across + spread_latent + shared_latent + scattered:
        copy.wait_send()
    for copy in locals_:
        copy.wait()
    for copy in swaps:
        copy.wait()


def front(query, turned, latent, key_w, value_w, out_w, residual, gain, gate, up, down):
    size = lax.axis_size("sp")
    depth, columns = gate.shape
    width = column_tiles(columns)[1] * 128
    own = (residual.shape[0] // lax.axis_size("tp"), residual.shape[1])
    wide = jax.ShapeDtypeStruct((size * depth, width), gate.dtype)
    tall = jax.ShapeDtypeStruct((width, size * down.shape[1]), down.dtype)
    dma = pltpu.SemaphoreType.DMA
    pairs = dma((3, size - 1))
    line = dma((size - 1,))
    here = pl.BlockSpec(memory_space=pltpu.VMEM)
    away = pl.BlockSpec(memory_space=pl.ANY)
    return pl.pallas_call(
        functools.partial(front_kernel, size, columns),
        out_shape=(
            wide, wide, tall,
            jax.ShapeDtypeStruct(own, jnp.float32), jax.ShapeDtypeStruct(own, jnp.bfloat16),
        ),
        in_specs=[here] * 8 + [away] * 3,
        out_specs=[away] * 3 + [here] * 2,
        scratch_shapes=[
            pltpu.VMEM((size,) + latent.shape, jnp.bfloat16),
            pltpu.VMEM((4,) + own, jnp.bfloat16),
            pltpu.VMEM((3,) + own, jnp.bfloat16),
            dma((3, 2)), pairs, pairs, pairs, pairs, line, line, line, line, dma((3,)), dma((3,)),
        ],
        compiler_params=pltpu.CompilerParams(collective_id=0, has_side_effects=True),
        name="front",
    )(query, turned, latent, key_w, value_w, out_w, residual, gain, gate, up, down)


def turn_lanes(vectors, positions):
    lanes = vectors.shape[1]
    freqs = ROPE // 4
    lane = jnp.arange(lanes, dtype=jnp.int32)
    inverse = jnp.power(10000.0, -(lane % freqs).astype(jnp.float32) / freqs)
    first_axis = lane % ROPE < ROPE // 2
    first_half = lane % (2 * freqs) < freqs
    place = jnp.where(
        first_axis[None], (positions // GRID_W)[:, None], (positions % GRID_W)[:, None]
    )
    angles = place.astype(jnp.float32) * inverse[None]
    partner = jnp.where(first_half, lane + freqs, lane - freqs)
    sign = jnp.where(first_half, -1.0, 1.0)
    swap = jnp.where(lane[:, None] == partner[None], sign[None], 0.0).astype(vectors.dtype)
    other = jnp.dot(vectors, swap, preferred_element_type=jnp.float32)
    turned = vectors.astype(jnp.float32) * jnp.cos(angles) + other * jnp.sin(angles)
    return turned.astype(jnp.bfloat16)


def spread_layer(
    query_nope, query_rope, token_latent, key_rope, latent_norm_gain, key_w, value_w,
    residual, out_w, ffn_gain, gate_w, up_w, down_w,
):
    rows = query_nope.shape[0]
    positions = lax.axis_index("sp") * rows + jnp.arange(rows, dtype=jnp.int32)
    repeats = query_rope.shape[1] // ROPE
    turned = turn_lanes(query_rope, positions)
    key_turned = turn_lanes(jnp.tile(key_rope, (1, repeats)), positions)
    latent = norm_rows(token_latent, latent_norm_gain).astype(jnp.bfloat16)
    packed = jnp.concatenate([latent, key_turned], axis=1)
    gate, up, down, mixed, normed = front(
        query_nope, turned, packed, key_w, value_w, out_w, residual, ffn_gain[None],
        gate_w, up_w, down_w,
    )
    return spread_ffn(normed, mixed, (gate, up, down), gate_w.shape[1])


def ffn_kernel(
    size, own, gate_w, up_w, down_w, keep, mixed, out,
    tokens, parts, from_core, from_x, from_z, total,
    z_send, z_recv, x_send, x_recv, c_send, c_recv,
    rc_send, rc_recv, rx_send, rx_recv, rz_send, rz_recv,
):
    here = lax.axis_index("sp")
    t = lax.axis_index("tp")
    core = t + 1 - 2 * lax.rem(t, 2)
    across = t + 2 - 4 * lax.div(t, 2)
    diagonal = core + 2 - 4 * lax.div(core, 2)
    rows = own.shape[0]
    to_core, to_x = {"tp": core}, {"tp": across}
    signal_all(
        [{"sp": lax.rem(here + shift, size)} for shift in range(1, size)] + [to_core, to_x]
    )
    z_copies = [None]
    for shift in range(1, size):
        copy = remote(
            own,
            tokens.at[here, t],
            z_send.at[shift],
            z_recv.at[shift],
            {"sp": lax.rem(here + shift, size)},
        )
        copy.start()
        z_copies.append(copy)
    tokens[here, t] = own[...]
    origins = [lax.rem(here - i + size, size) for i in range(size)]
    pending = []
    x_copies, c_first, c_second, r_first, r_second, rx, rz = {}, {}, {}, {}, {}, {}, {}

    def start(table, i, *args):
        copy = remote(*args)
        copy.start()
        table[i] = copy
        pending.append(copy)

    def step_a(i):
        o = origins[i]
        if i:
            z_copies[i].wait_recv()
        block = tokens.at[o, t] if i else own
        start(x_copies, i, block, tokens.at[o, t], x_send.at[i], x_recv.at[i], to_x)
        start(c_first, i, block, tokens.at[o, t], c_send.at[i, 0], c_recv.at[i, 0], to_core)

    def step_b(i):
        o = origins[i]
        x_copies[i].wait_recv()
        block = tokens.at[o, across]
        start(c_second, i, block, block, c_send.at[i, 1], c_recv.at[i, 1], to_core)

    def step_c(i):
        o = origins[i]
        c_first[i].wait_recv()
        c_second[i].wait_recv()
        x = tokens[o].reshape(4 * rows, own.shape[1])
        gate = jnp.dot(x, gate_w[...], preferred_element_type=jnp.float32)
        up = jnp.dot(x, up_w[...], preferred_element_type=jnp.float32)
        hidden = (gate / (1.0 + jnp.exp(-gate)) * up * keep[...]).astype(jnp.bfloat16)
        step = 512
        for col in range(0, own.shape[1], step):
            term = jnp.dot(
                hidden, down_w[:, col : col + step], preferred_element_type=jnp.float32
            )
            parts[o, :, :, col : col + step] = term.astype(jnp.bfloat16).reshape(4, rows, step)
        start(r_first, i, parts.at[o, diagonal], from_core.at[i, 1], rc_send.at[i, 1], rc_recv.at[i, 1], to_core)
        start(r_second, i, parts.at[o, core], from_core.at[i, 0], rc_send.at[i, 0], rc_recv.at[i, 0], to_core)

    def plus(one, two):
        return one.astype(jnp.float32) + two.astype(jnp.float32)

    def step_d(i):
        o = origins[i]
        r_first[i].wait_recv()
        parts[o, across] = plus(parts[o, across], from_core[i, 1]).astype(jnp.bfloat16)
        start(rx, i, parts.at[o, across], from_x.at[i], rx_send.at[i], rx_recv.at[i], to_x)
        r_second[i].wait_recv()
        parts[o, t] = plus(parts[o, t], from_core[i, 0]).astype(jnp.bfloat16)

    def step_e(i):
        o = origins[i]
        rx[i].wait_recv()
        if i == 0:
            total[...] = mixed[...] + plus(parts[o, t], from_x[i])
            return
        parts[o, t] = plus(parts[o, t], from_x[i]).astype(jnp.bfloat16)
        start(rz, i, parts.at[o, t], from_z.at[i], rz_send.at[i], rz_recv.at[i], {"sp": o})

    steps = {"a": step_a, "b": step_b, "c": step_c, "d": step_d, "e": step_e}
    last = size - 1
    order = [("a", 0)]
    for i in range(size + 1):
        for name, lag in (("a", -1), ("b", 0), ("c", 0), ("d", 0), ("e", 1)):
            if 0 <= i - lag <= last:
                order.append((name, i - lag))
    for name, i in order:
        steps[name](i)
    result = total[...]
    for i in range(1, size):
        rz[i].wait_recv()
        result = result + from_z[i].astype(jnp.float32)
    out[...] = result.astype(out.dtype)
    for copy in z_copies[1:] + pending:
        copy.wait_send()


def spread_ffn(normed_own, mixed_own, swapped, hidden_columns):
    size = lax.axis_size("sp")
    here = lax.axis_index("sp")
    per = column_tiles(hidden_columns)[1]
    before = jnp.where(here > 0, window_start(jnp.maximum(here - 1, 0), hidden_columns) + per, 0)
    first = (before - window_start(here, hidden_columns)) * 128
    keep = (jnp.arange(per * 128, dtype=jnp.int32) >= first).astype(jnp.float32)[None]
    block = normed_own.shape
    dma = pltpu.SemaphoreType.DMA
    vmem = lambda *lead: pltpu.VMEM(lead + block, jnp.bfloat16)
    pair = [dma((size,)), dma((size,))]
    double = [dma((size, 2)), dma((size, 2))]
    return pl.pallas_call(
        functools.partial(ffn_kernel, size),
        out_shape=jax.ShapeDtypeStruct(block, jnp.bfloat16),
        in_specs=[pl.BlockSpec(memory_space=pltpu.VMEM)] * 6,
        out_specs=pl.BlockSpec(memory_space=pltpu.VMEM),
        scratch_shapes=[
            vmem(size, 4), vmem(size, 4), vmem(size, 2), vmem(size), vmem(size),
            pltpu.VMEM(block, jnp.float32),
        ] + pair + pair + double + double + pair + pair,
        compiler_params=pltpu.CompilerParams(collective_id=1, has_side_effects=True),
        name="spread_ffn",
    )(normed_own, *swapped, keep, mixed_own)


def local(
    query_nope,
    query_rope,
    token_latent,
    key_rope,
    latent_norm_gain,
    key_expand_weight,
    value_expand_weight,
    residual,
    out_weight,
    ffn_gain,
    gate_weight,
    up_weight,
    down_weight,
):
    if spread_hidden(query_nope.shape[0] * lax.axis_size("sp"), gate_weight.shape[1]):
        return spread_layer(
            query_nope,
            query_rope,
            token_latent,
            key_rope,
            latent_norm_gain,
            key_expand_weight,
            value_expand_weight,
            residual,
            out_weight,
            ffn_gain,
            gate_weight,
            up_weight,
            down_weight,
        )
    tok_rows = query_nope.shape[0]
    heads_here = query_nope.shape[1] // UNROTATED_SIZE
    own_rows = tok_rows // lax.axis_size("tp")
    tp_index = lax.axis_index("tp")
    positions = lax.axis_index("sp") * tok_rows + jnp.arange(tok_rows, dtype=jnp.int32)
    query_flat = query_nope.reshape(tok_rows, heads_here, UNROTATED_SIZE)
    query_turned = turn_heads(
        query_rope.astype(jnp.float32).reshape(tok_rows, heads_here, ROPE), positions
    ).astype(jnp.bfloat16)
    latent = norm_rows(token_latent, latent_norm_gain).astype(jnp.bfloat16)
    key_turned = turn_heads(key_rope.astype(jnp.float32)[:, None, :], positions)[:, 0].astype(
        jnp.bfloat16
    )
    key_cols = lax.dynamic_slice_in_dim(
        key_expand_weight, tp_index * heads_here * UNROTATED_SIZE, heads_here * UNROTATED_SIZE, 1
    )
    value_cols = lax.dynamic_slice_in_dim(
        value_expand_weight, tp_index * heads_here * VALUE_SIZE, heads_here * VALUE_SIZE, 1
    )
    score_scale = (UNROTATED_SIZE + ROPE) ** (-0.5)

    def absorb(carried, block_in):
        latent_block, rope_block = block_in
        block_rows = latent_block.shape[0]
        key_rows = jnp.dot(latent_block, key_cols, preferred_element_type=jnp.float32).astype(
            jnp.bfloat16
        )
        key_rows = key_rows.reshape(block_rows, heads_here, UNROTATED_SIZE)
        value_rows = jnp.dot(latent_block, value_cols, preferred_element_type=jnp.float32).astype(
            jnp.bfloat16
        )
        value_rows = value_rows.reshape(block_rows, heads_here, VALUE_SIZE)
        scores = (
            jnp.einsum("qhd,khd->hqk", query_flat, key_rows, preferred_element_type=jnp.float32)
            + jnp.einsum(
                "qhd,kd->hqk", query_turned, rope_block, preferred_element_type=jnp.float32
            )
        ) * score_scale
        highest, totals, accumulated = carried
        new_highest = jnp.maximum(highest, jnp.max(scores, axis=-1))
        shrink = jnp.exp(highest - new_highest)
        weights = jnp.exp(scores - new_highest[:, :, None])
        totals = totals * shrink + jnp.sum(weights, axis=-1)
        accumulated = accumulated * shrink.T[:, :, None] + jnp.einsum(
            "hqk,khd->qhd",
            weights.astype(jnp.bfloat16),
            value_rows,
            preferred_element_type=jnp.float32,
        )
        return ((new_highest, totals, accumulated), None)

    initial = (
        jnp.full((heads_here, tok_rows), -jnp.inf, jnp.float32),
        jnp.zeros((heads_here, tok_rows), jnp.float32),
        jnp.zeros((tok_rows, heads_here, VALUE_SIZE), jnp.float32),
    )
    carried = initial
    latent_piece = lax.all_gather(latent, "sp", axis=0, tiled=True)
    rope_piece = lax.all_gather(key_turned, "sp", axis=0, tiled=True)
    shard_count = latent_piece.shape[0] // tok_rows
    grouped = max(
        (
            factor
            for factor in range(1, shard_count + 1)
            if shard_count % factor == 0 and factor * tok_rows <= max(1024, tok_rows)
        )
    )
    block_rows = grouped * tok_rows
    blocks = (
        latent_piece.reshape(-1, block_rows, latent_piece.shape[1]),
        rope_piece.reshape(-1, block_rows, rope_piece.shape[1]),
    )
    carried, _ = lax.scan(absorb, carried, blocks)
    highest, totals, accumulated = carried
    attended = (
        (accumulated / totals.T[:, :, None])
        .reshape(tok_rows, heads_here * VALUE_SIZE)
        .astype(jnp.bfloat16)
    )
    projected = jnp.dot(attended, out_weight, preferred_element_type=jnp.float32).astype(
        jnp.bfloat16
    )
    summed = lax.psum(projected, "tp").astype(jnp.float32)
    mixed_all = residual.astype(jnp.float32) + summed
    normed_all = norm_rows(mixed_all, ffn_gain).astype(jnp.bfloat16)
    mixed_own = lax.dynamic_slice_in_dim(mixed_all, tp_index * own_rows, own_rows, 0)
    gate_piece = lax.all_gather(gate_weight, "sp", axis=0, tiled=True)
    up_piece = lax.all_gather(up_weight, "sp", axis=0, tiled=True)
    gate = jnp.dot(normed_all, gate_piece, preferred_element_type=jnp.float32)
    up_part = jnp.dot(normed_all, up_piece, preferred_element_type=jnp.float32)
    hidden = (jax.nn.silu(gate) * up_part).astype(jnp.bfloat16)
    terms = jnp.dot(
        hidden,
        lax.all_gather(down_weight, "sp", axis=1, tiled=True),
        preferred_element_type=jnp.float32,
    )
    ffn_own = lax.psum_scatter(
        terms.astype(jnp.bfloat16), "tp", scatter_dimension=0, tiled=True
    ).astype(jnp.float32)
    return (mixed_own + ffn_own).astype(jnp.bfloat16)


def solution(mesh):
    return jax.shard_map(
        local,
        mesh=mesh,
        in_specs=(
            P(("grp", "sp"), "tp"),
            P(("grp", "sp"), "tp"),
            P(("grp", "sp"), None),
            P(("grp", "sp"), None),
            P(),
            P(),
            P(),
            P(("grp", "sp"), None),
            P("tp", None),
            P(),
            P("sp", "tp"),
            P("sp", "tp"),
            P("tp", "sp"),
        ),
        out_specs=P(("grp", "sp", "tp"), None),
        check_vma=False,
    )
```
